32 devices in a mesh: kv: 4 (over y, x), tp: 8 (over z, core).
Axes of the slice: x: 2, y: 2, z: 4, core: 2. Of those that a mesh axis runs over, the one named last changes fastest.
Arguments:
- tokens: bfloat16 [256, 4096], P(None, ('kv', 'tp')), may hold values from -10 to 10
- past_state: float32 [256, 32, 64, 128], P('kv', 'tp'), may hold values from -6 to 6
- first_gain: float32 [4096], P('kv'), may hold values from 0.1 to 1.9
- first_gate: bfloat16 [4096, 11264], P('kv', 'tp'), may hold values from -0.09375 to 0.09375
- first_up: bfloat16 [4096, 11264], P('kv', 'tp'), may hold values from -0.09375 to 0.09375
- first_down: bfloat16 [11264, 4096], P('tp', 'kv'), may hold values from -0.078125 to 0.078125
- mix_gain: float32 [4096], P('kv'), may hold values from 0.1 to 1.9
- query_weight: bfloat16 [4096, 2048], P('kv', 'tp'), may hold values from -0.09375 to 0.09375
- key_weight: bfloat16 [4096, 2048], P('kv', 'tp'), may hold values from -0.09375 to 0.09375
- value_weight: bfloat16 [4096, 4096], P('kv', 'tp'), may hold values from -0.09375 to 0.09375
- output_gate_weight: bfloat16 [4096, 4096], P('kv', 'tp'), may hold values from -0.09375 to 0.09375
- head_gain: float32 [4096], P('tp'), may hold values from 0.1 to 1.9
- out_weight: bfloat16 [4096, 4096], P('tp', 'kv'), may hold values from -0.125 to 0.125
- second_gain: float32 [4096], P('kv'), may hold values from 0.1 to 1.9
- second_gate: bfloat16 [4096, 11264], P('kv', 'tp'), may hold values from -0.09375 to 0.09375
- second_up: bfloat16 [4096, 11264], P('kv', 'tp'), may hold values from -0.09375 to 0.09375
- second_down: bfloat16 [11264, 4096], P('tp', 'kv'), may hold values from -0.078125 to 0.078125
Outputs:
- mixed: bfloat16 [256, 4096], P(None, ('kv', 'tp'))
- new_state: float32 [256, 32, 64, 128], P('kv', 'tp')
The draws below stay inside these ranges and needn't reach their ends.
All inputs are finite; a program needn't handle non-finite values.
Results may differ from the reference program's by a relative error of at most 0.033.
Values may be sent and summed in bfloat16 or wider, within the bound.
A program may use at most 128 MiB of HBM per device.

```python
import jax
import jax.numpy as jnp
from jax import lax

D = 4096
HEADS = 32
HEAD_K = 64
HEAD_V = 128
FF = 11264
POS = 16384
BATCH = 256
XCOLS = 128


def draw_tokens(key, part):
    key_values, key_scales, key_common = jax.random.split(key, 3)
    block_count = D // XCOLS
    block_scale = jnp.exp(jax.random.uniform(key_scales, (block_count,), jnp.float32, jnp.log(0.35), jnp.log(2.0)))
    column_scale = jnp.repeat(block_scale, XCOLS)
    values = jnp.clip(jax.random.normal(key_values, (BATCH, D), jnp.float32), -5.0, 5.0)
    return (values * column_scale[None, :]).astype(jnp.bfloat16)


def spiked(values, stream_key, source, target, blocks, factor):
    def block_of(position):
        return (jnp.arange(values.shape[position]) // (values.shape[position] // blocks)).reshape((-1,) + (1,) * (values.ndim - 1 - position))

    one_side = jax.random.permutation(stream_key, blocks)[block_of(target)]
    other_side = (block_of(target) + blocks // 2) % blocks
    return jnp.where((block_of(source) == one_side) | (block_of(source) == other_side), factor * values, values)


def block_levels(rng, extent, shards, least, largest):
    level, own = 1.0, jax.random.fold_in(rng, 6)
    for axis_at, shards_of in shards:
        heights = jnp.exp(jax.random.uniform(jax.random.fold_in(own, axis_at), (shards_of,), jnp.float32, least / len(shards), largest / len(shards)))
        level = level * jnp.repeat(heights, extent[axis_at] // shards_of).reshape([-1 if axis == axis_at else 1 for axis in range(len(extent))])
    return level


def noise(rng, extent, scale, reach, cuts=(), kind=jnp.bfloat16):
    loudness = block_levels(rng, extent, cuts, -0.22, 0.18) if cuts else 1.0
    array = jax.random.normal(rng, extent, jnp.float32) * scale * loudness
    return jnp.minimum(jnp.maximum(array, -reach), reach).astype(kind)


def bell_draw_with(rng, dims, scale, reach, shards, heavy, kind=jnp.bfloat16):
    drawn = scale * jax.random.normal(rng, dims, jnp.float32)
    if shards:
        drawn = drawn * block_levels(rng, dims, shards, -0.22, 0.18)
    return jnp.clip(spiked(drawn, jax.random.fold_in(rng, 3), *heavy), -reach, reach).astype(kind)


def setup_inputs(seed: int = 0) -> dict:
    streams_of = jax.random.split(jax.random.key(seed), 18)
    tokens = draw_tokens(jax.random.fold_in(streams_of[17], 71), 0)
    past_state = noise(streams_of[1], (BATCH, HEADS, HEAD_K, HEAD_V), 1.0, 6.0, ((0, 4), (1, 8)), jnp.float32)
    first_gain = jnp.clip(1.0 + 0.18 * jax.random.normal(streams_of[2], (D,), jnp.float32), 0.1, 1.9)
    first_gate = noise(streams_of[3], (D, FF), D ** -0.5, 0.09375, ((0, 4), (1, 8)))
    first_up = noise(streams_of[4], (D, FF), D ** -0.5, 0.09375, ((0, 4), (1, 8)))
    first_down = bell_draw_with(streams_of[5], (FF, D), FF ** -0.5, 0.078125, ((0, 8), (1, 4)), (0, 1, 8, 2.0))
    mix_gain = jnp.clip(1.0 + 0.18 * jax.random.normal(streams_of[6], (D,), jnp.float32), 0.1, 1.9)
    query_weight = noise(streams_of[7], (D, HEADS * HEAD_K), D ** -0.5, 0.09375, ((0, 4), (1, 8)))
    key_weight = noise(streams_of[8], (D, HEADS * HEAD_K), D ** -0.5, 0.09375, ((0, 4), (1, 8)))
    value_weight = noise(streams_of[9], (D, HEADS * HEAD_V), D ** -0.5, 0.09375, ((0, 4), (1, 8)))
    output_gate_weight = noise(streams_of[10], (D, HEADS * HEAD_V), D ** -0.5, 0.09375, ((0, 4), (1, 8)))
    head_gain = jnp.clip(1.0 + 0.18 * jax.random.normal(streams_of[11], (HEADS * HEAD_V,), jnp.float32), 0.1, 1.9)
    out_weight = bell_draw_with(streams_of[12], (HEADS * HEAD_V, D), (HEADS * HEAD_V) ** -0.5, 0.125, ((0, 8), (1, 4)), (0, 1, 8, 2.0))
    second_gain = jnp.clip(1.0 + 0.18 * jax.random.normal(streams_of[13], (D,), jnp.float32), 0.1, 1.9)
    second_gate = noise(streams_of[14], (D, FF), D ** -0.5, 0.09375, ((0, 4), (1, 8)))
    second_up = noise(streams_of[15], (D, FF), D ** -0.5, 0.09375, ((0, 4), (1, 8)))
    second_down = bell_draw_with(streams_of[16], (FF, D), FF ** -0.5, 0.078125, ((0, 8), (1, 4)), (0, 1, 8, 2.0))
    return {"tokens": tokens, "past_state": past_state, "first_gain": first_gain, "first_gate": first_gate, "first_up": first_up, "first_down": first_down, "mix_gain": mix_gain, "query_weight": query_weight, "key_weight": key_weight, "value_weight": value_weight, "output_gate_weight": output_gate_weight, "head_gain": head_gain, "out_weight": out_weight, "second_gain": second_gain, "second_gate": second_gate, "second_up": second_up, "second_down": second_down}


EPS_RMS = 1e-06
EPS_GROUP = 1e-05
ROPE_BASE = 10000.0

def rotate(vectors):
    half_width = vectors.shape[-1] // 2
    frequency = ROPE_BASE ** (-jnp.arange(half_width, dtype=jnp.float32) / half_width)
    angles = POS * frequency
    cosine = jnp.cos(angles)
    sine_part = jnp.sin(angles)
    lower = vectors[..., :half_width]
    upper = vectors[..., half_width:]
    return jnp.concatenate([lower * cosine - upper * sine_part, lower * sine_part + upper * cosine], axis=-1)

def row_factor(resid_f):
    return lax.rsqrt(lax.optimization_barrier(jnp.sum(resid_f * resid_f, axis=1)) / D + EPS_RMS)[:, None]

def channel_mix(resid, gain, w_gate, w_up, w_down):
    resid_f = resid.astype(jnp.float32)
    inverse_rms = row_factor(resid_f)
    scaled = (resid_f * gain).astype(jnp.bfloat16)
    gate_sum = jnp.dot(scaled, w_gate, preferred_element_type=jnp.float32) * inverse_rms
    up_sum = jnp.dot(scaled, w_up, preferred_element_type=jnp.float32) * inverse_rms
    hidden = (jax.nn.silu(gate_sum) * up_sum).astype(jnp.bfloat16)
    branch = jnp.dot(hidden, w_down, preferred_element_type=jnp.float32)
    return (resid_f + 0.5 * branch).astype(jnp.bfloat16)

def token_mix(resid, past_state, gain, query_weight, key_weight, value_weight, output_gate_weight, head_gain, out_weight):
    resid_f = resid.astype(jnp.float32)
    row_total = resid.shape[0]
    inverse_rms = row_factor(resid_f)
    scaled = (resid_f * gain).astype(jnp.bfloat16)
    queries = jnp.dot(scaled, query_weight, preferred_element_type=jnp.float32) * inverse_rms
    keys_now = jnp.dot(scaled, key_weight, preferred_element_type=jnp.float32) * inverse_rms
    values_now = jnp.dot(scaled, value_weight, preferred_element_type=jnp.float32) * inverse_rms
    gate_now = jnp.dot(scaled, output_gate_weight, preferred_element_type=jnp.float32) * inverse_rms
    queries = rotate(queries.reshape(row_total, HEADS, HEAD_K)) * HEAD_K ** (-0.5)
    keys_now = rotate(keys_now.reshape(row_total, HEADS, HEAD_K))
    values_now = values_now.reshape(row_total, HEADS, HEAD_V)
    head_level = jnp.arange(HEADS, dtype=jnp.float32)
    retained = 1.0 - jnp.exp2(-5.0 - 16.0 * head_level / (HEADS - 1))
    new_state = retained[None, :, None, None] * past_state + keys_now[:, :, :, None] * values_now[:, :, None, :]
    retrieved = jnp.einsum('bhk,bhkv->bhv', queries, new_state, precision=lax.Precision.HIGHEST)
    head_mean = lax.optimization_barrier(jnp.mean(retrieved, axis=-1, keepdims=True))
    variance = lax.optimization_barrier(jnp.mean(jnp.square(retrieved - head_mean), axis=-1, keepdims=True))
    normed = ((retrieved - head_mean) * lax.rsqrt(variance + EPS_GROUP)).reshape(row_total, HEADS * HEAD_V) * head_gain
    mixed_heads = (jax.nn.silu(gate_now) * normed).astype(jnp.bfloat16)
    branch = jnp.dot(mixed_heads, out_weight, preferred_element_type=jnp.float32)
    return ((resid_f + branch).astype(jnp.bfloat16), new_state)

def reference(tokens, past_state, first_gain, first_gate, first_up, first_down, mix_gain, query_weight, key_weight, value_weight, output_gate_weight, head_gain, out_weight, second_gain, second_gate, second_up, second_down):
    first = channel_mix(tokens, first_gain, first_gate, first_up, first_down)
    second, new_state = token_mix(first, past_state, mix_gain, query_weight, key_weight, value_weight, output_gate_weight, head_gain, out_weight)
    mixed = channel_mix(second, second_gain, second_gate, second_up, second_down)
    return (mixed, new_state)
```

```python
import jax
import jax.numpy as jnp
from jax import lax
from jax.experimental import pallas as pl
from jax.experimental.pallas import tpu as pltpu
from jax.sharding import PartitionSpec as P

D = 4096
HEADS = 32
HEAD_K = 64
HEAD_V = 128
POS = 16384


EPS_RMS = 1e-06
EPS_GROUP = 1e-05
ROPE_BASE = 10000.0


def rotate(vectors):
    half_width = vectors.shape[-1] // 2
    frequency = ROPE_BASE ** (-jnp.arange(half_width, dtype=jnp.float32) / half_width)
    angles = POS * frequency
    cosine = jnp.cos(angles)
    sine_part = jnp.sin(angles)
    lower = vectors[..., :half_width]
    upper = vectors[..., half_width:]
    return jnp.concatenate(
        [lower * cosine - upper * sine_part, lower * sine_part + upper * cosine], axis=-1
    )


def activate(gate_sum, up_sum, summed):
    inverse_rms = lax.rsqrt(summed / D + EPS_RMS)[:, None]
    return (jax.nn.silu(gate_sum * inverse_rms) * (up_sum * inverse_rms)).astype(jnp.bfloat16)


def channel_mix(widened, gain, w_gate, w_up, w_down):
    widened_f = widened.astype(jnp.float32)
    scaled = (widened_f * gain).astype(jnp.bfloat16)
    squares = jnp.sum(widened_f * widened_f, axis=1)
    gate_part = jnp.dot(scaled, w_gate, preferred_element_type=jnp.float32)
    up_part = jnp.dot(scaled, w_up, preferred_element_type=jnp.float32)
    gate_sum, up_sum, summed = (
        lax.psum(gate_part.astype(jnp.bfloat16), "kv").astype(jnp.float32),
        lax.psum(up_part.astype(jnp.bfloat16), "kv").astype(jnp.float32),
        lax.psum(squares.astype(jnp.bfloat16), "kv").astype(jnp.float32),
    )
    return 0.5 * jnp.dot(
        activate(gate_sum, up_sum, summed), w_down, preferred_element_type=jnp.float32
    )


def token_mix(
    widened,
    past_state,
    gain,
    query_weight,
    key_weight,
    value_weight,
    output_gate_weight,
    head_gain,
    out_weight,
):
    widened_f = widened.astype(jnp.float32)
    scaled = (widened_f * gain).astype(jnp.bfloat16)
    squares = jnp.sum(widened_f * widened_f, axis=1)
    query_part = jnp.dot(scaled, query_weight, preferred_element_type=jnp.float32)
    key_part = jnp.dot(scaled, key_weight, preferred_element_type=jnp.float32)
    value_part = jnp.dot(scaled, value_weight, preferred_element_type=jnp.float32)
    gate_part = jnp.dot(scaled, output_gate_weight, preferred_element_type=jnp.float32)
    queries, keys_now, values_now, gate_now, summed = (
        lax.psum_scatter(
            query_part.astype(jnp.bfloat16), "kv", scatter_dimension=0, tiled=True
        ).astype(jnp.float32),
        lax.psum_scatter(
            key_part.astype(jnp.bfloat16), "kv", scatter_dimension=0, tiled=True
        ).astype(jnp.float32),
        lax.psum_scatter(
            value_part.astype(jnp.bfloat16), "kv", scatter_dimension=0, tiled=True
        ).astype(jnp.float32),
        lax.psum_scatter(
            gate_part.astype(jnp.bfloat16), "kv", scatter_dimension=0, tiled=True
        ).astype(jnp.float32),
        lax.psum_scatter(
            squares.astype(jnp.bfloat16), "kv", scatter_dimension=0, tiled=True
        ).astype(jnp.float32),
    )
    inverse_rms = lax.rsqrt(summed / D + EPS_RMS)[:, None]
    row_count = past_state.shape[0]
    local_heads = past_state.shape[1]
    queries = rotate((queries * inverse_rms).reshape(row_count, local_heads, HEAD_K)) * HEAD_K ** (
        -0.5
    )
    keys_now = rotate((keys_now * inverse_rms).reshape(row_count, local_heads, HEAD_K))
    values_now = (values_now * inverse_rms).reshape(row_count, local_heads, HEAD_V)
    gate_now = gate_now * inverse_rms
    head_level = (lax.axis_index("tp") * local_heads + jnp.arange(local_heads)).astype(jnp.float32)
    retained = 1.0 - jnp.exp2(-5.0 - 16.0 * head_level / (HEADS - 1))
    new_state = (
        retained[None, :, None, None] * past_state
        + keys_now[:, :, :, None] * values_now[:, :, None, :]
    )
    retrieved = jnp.einsum("bhk,bhkv->bhv", queries, new_state, precision=lax.Precision.HIGHEST)
    head_mean = jnp.mean(retrieved, axis=-1, keepdims=True)
    variance = jnp.mean(jnp.square(retrieved - head_mean), axis=-1, keepdims=True)
    normed = ((retrieved - head_mean) * lax.rsqrt(variance + EPS_GROUP)).reshape(
        row_count, local_heads * HEAD_V
    )
    mixed_heads = (jax.nn.silu(gate_now) * (normed * head_gain)).astype(jnp.bfloat16)
    projected = jnp.dot(
        lax.all_gather(mixed_heads, "kv", axis=0, tiled=True),
        out_weight,
        preferred_element_type=jnp.float32,
    )
    return (projected, new_state)


def shards(
    tokens,
    past_state,
    first_gain,
    first_gate,
    first_up,
    first_down,
    mix_gain,
    query_weight,
    key_weight,
    value_weight,
    output_gate_weight,
    head_gain,
    out_weight,
    second_gain,
    second_gate,
    second_up,
    second_down,
):

    def first_section(widened):
        return (channel_mix(widened, first_gain, first_gate, first_up, first_down), None)

    def middle_section(widened):
        return token_mix(
            widened,
            past_state,
            mix_gain,
            query_weight,
            key_weight,
            value_weight,
            output_gate_weight,
            head_gain,
            out_weight,
        )

    def last_section(widened):
        return (channel_mix(widened, second_gain, second_gate, second_up, second_down), None)

    sections = [first_section, middle_section, last_section]
    own_columns = tokens
    widened = lax.all_gather(tokens, "tp", axis=1, tiled=True)
    state_out = past_state
    for section_index in range(3):
        branch_out, produced = sections[section_index](widened)
        if produced is not None:
            state_out = produced
        own_piece = lax.psum_scatter(
            branch_out.astype(jnp.bfloat16), "tp", scatter_dimension=1, tiled=True
        ).astype(jnp.float32)
        own_columns = (own_columns.astype(jnp.float32) + own_piece).astype(jnp.bfloat16)
        if section_index < 2:
            widened = lax.all_gather(own_columns, "tp", axis=1, tiled=True)
    return (own_columns, state_out)


MESH = pl.DeviceIdType.MESH
LANES = 128
F32 = jnp.float32
BF16 = jnp.bfloat16
VMEM_BYTES = 60 * 1024 * 1024


def send(src, dst, send_sem, recv_sem, target):
    copy = pltpu.make_async_remote_copy(
        src_ref=src,
        dst_ref=dst,
        send_sem=send_sem,
        recv_sem=recv_sem,
        device_id=target,
        device_id_type=MESH,
    )
    copy.start()
    return copy


class Place:
    def __init__(self, groups, width):
        self.groups, self.width, self.chips = groups, width, width // 2
        self.kv = lax.axis_index("kv")
        self.tp = lax.axis_index("tp")
        self.chip = self.tp // 2
        self.core = lax.rem(self.tp, 2)
        self.partner = {"tp": 2 * self.chip + 1 - self.core}

    def chip_peer(self, d):
        return lax.rem(self.chip + d, self.chips)

    def tp_peer(self, d):
        return {"tp": 2 * self.chip_peer(d) + self.core}

    def tp_origin(self, d):
        return 2 * lax.rem(self.chip + self.chips - d, self.chips) + self.core

    def kv_index(self, d):
        return lax.rem(self.kv + d, self.groups)

    def kv_peer(self, d):
        return {"kv": self.kv_index(d)}

    def barrier(self):
        barrier = pltpu.get_barrier_semaphore()
        targets = [self.partner]
        targets += [self.tp_peer(d) for d in range(1, self.chips)]
        targets += [self.kv_peer(d) for d in range(1, self.groups)]
        for target in targets:
            pl.semaphore_signal(barrier, inc=1, device_id=target, device_id_type=MESH)
        pl.semaphore_wait(barrier, len(targets))


def gather_scratch(place_shape, rows, cols):
    groups, width = place_shape
    chips = width // 2
    sems = [pltpu.SemaphoreType.DMA((chips,))] * 4
    return [pltpu.VMEM((width, rows, cols), BF16)] + sems


def gather_tp(place, own, scratch):
    blocks, send_far, recv_far, send_near, recv_near = scratch
    me = place.tp
    far = [
        send(own, blocks.at[me], send_far.at[d], recv_far.at[d], place.tp_peer(d))
        for d in range(1, place.chips)
    ]
    near = [send(own, blocks.at[me], send_near.at[0], recv_near.at[0], place.partner)]
    blocks[me] = own[...]
    for d in range(1, place.chips):
        far[d - 1].wait_recv()
        block = blocks.at[place.tp_origin(d)]
        near.append(send(block, block, send_near.at[d], recv_near.at[d], place.partner))
    for copy in near:
        copy.wait_recv()
    for copy in far + near:
        copy.wait_send()
    return blocks


def scale_scratch(place_shape, rows, cols):
    groups, width = place_shape
    sems = [pltpu.SemaphoreType.DMA((groups,))] * 2
    return [
        pltpu.VMEM((rows, width * cols), BF16),
        pltpu.VMEM((groups, rows // groups, LANES), BF16),
        pltpu.VMEM((groups, rows // groups, LANES), BF16),
    ] + sems


def scale(place, blocks, gain, scratch):
    scaled, sq_out, sq_in, send_sem, recv_sem = scratch
    width, rows, cols = blocks.shape
    part = rows // place.groups
    total = jnp.zeros((rows, 1), F32)
    for t in range(width):
        block = blocks[t].astype(F32)
        at = slice(t * cols, (t + 1) * cols)
        scaled[:, at] = (block * gain[:, at]).astype(BF16)
        total = total + jnp.sum(block * block, axis=1, keepdims=True)
    high = total.astype(BF16).astype(F32)
    low = total - high
    lane = lax.broadcasted_iota(jnp.int32, (rows, LANES), 1)
    both = jnp.where(lane < LANES // 2, high, low).astype(BF16)
    for k in range(place.groups):
        sq_out[k] = both[k * part : (k + 1) * part]
    copies = [
        send(
            sq_out.at[place.kv_index(d)],
            sq_in.at[d],
            send_sem.at[d],
            recv_sem.at[d],
            place.kv_peer(d),
        )
        for d in range(1, place.groups)
    ]

    def inverse_rms():
        for copy in copies:
            copy.wait()
        both = sq_out[place.kv].astype(F32)
        for d in range(1, place.groups):
            both = both + sq_in[d].astype(F32)
        summed = jnp.sum(both, axis=1, keepdims=True) / (LANES // 2)
        return lax.rsqrt(summed / D + EPS_RMS)

    return scaled, inverse_rms


def spans(count, pieces):
    cuts = [count * i // pieces for i in range(pieces + 1)]
    return [(a, b) for a, b in zip(cuts, cuts[1:]) if b > a]


FF_PIECES = 3


def hidden_scratch(place_shape, rows, units):
    groups, width = place_shape
    part, tiles = rows // groups, units // LANES
    exchange = pltpu.VMEM((groups, tiles, 2, part, LANES), BF16)
    sems = [pltpu.SemaphoreType.DMA((FF_PIECES, groups))] * 4
    return [exchange, exchange, pltpu.VMEM((rows, units), BF16)] + sems


def hidden_units(place, scaled, inverse_rms, w_gate, w_up, scratch):
    out, into, hidden, send_part, recv_part, send_hid, recv_hid = scratch
    rows, units = hidden.shape
    groups = place.groups
    part, tiles = rows // groups, units // LANES
    pieces = spans(tiles, FF_PIECES)
    own_rows = pl.ds(pl.multiple_of(place.kv * part, part), part)

    def lanes(j):
        return pl.ds(pl.multiple_of(j * LANES, LANES), LANES)

    def products(j, carry):
        weights = jnp.concatenate([w_gate[:, lanes(j)], w_up[:, lanes(j)]], axis=1)
        result = jnp.dot(scaled[...], weights, preferred_element_type=F32).astype(BF16)
        for k in range(groups):
            for side in range(2):
                out[k, j, side] = result[
                    k * part : (k + 1) * part, side * LANES : (side + 1) * LANES
                ]
        return carry

    part_copies = []
    for p, (low, high) in enumerate(pieces):
        lax.fori_loop(low, high, products, 0)
        span = pl.ds(low, high - low)
        part_copies.append(
            [
                send(
                    out.at[place.kv_index(d), span],
                    into.at[d, span],
                    send_part.at[p, d],
                    recv_part.at[p, d],
                    place.kv_peer(d),
                )
                for d in range(1, groups)
            ]
        )
    factor = inverse_rms()

    def activation(j, carry):
        sums = []
        for side in range(2):
            total = out[place.kv, j, side].astype(F32)
            for d in range(1, groups):
                total = total + into[d, j, side].astype(F32)
            sums.append(total * factor)
        value = sums[0] / (1.0 + jnp.exp(-sums[0])) * sums[1]
        hidden[own_rows, lanes(j)] = value.astype(BF16)
        return carry

    hid_copies = []
    for p, (low, high) in enumerate(pieces):
        for copy in part_copies[p]:
            copy.wait_recv()
        lax.fori_loop(low, high, activation, 0)
        block = hidden.at[own_rows, pl.ds(low * LANES, (high - low) * LANES)]
        hid_copies += [
            send(block, block, send_hid.at[p, d], recv_hid.at[p, d], place.kv_peer(d))
            for d in range(1, groups)
        ]
    for copies in part_copies:
        for copy in copies:
            copy.wait_send()
    for copy in hid_copies:
        copy.wait()
    return hidden


def branch_scratch(place_shape, rows, cols):
    groups, width = place_shape
    chips = width // 2
    half = (chips, rows, cols)
    sems = [pltpu.SemaphoreType.DMA((chips,))] * 2
    near = [pltpu.SemaphoreType.DMA] * 2
    return [
        pltpu.VMEM(half, BF16),
        pltpu.VMEM(half, BF16),
        pltpu.VMEM(half, F32),
        pltpu.VMEM(half, BF16),
        pltpu.VMEM(half, BF16),
    ] + near + sems


def branch(place, left, weight, factor, scratch):
    away, near_in, own, pair, far_in, send_near, recv_near, send_far, recv_far = scratch
    chips, rows, cols = away.shape

    def products(core, into):
        def step(i, carry):
            columns = [
                weight[:, pl.ds(pl.multiple_of((2 * (2 * i + s) + core) * cols, cols), cols)]
                for s in range(2)
            ]
            result = factor * jnp.dot(
                left[...], jnp.concatenate(columns, axis=1), preferred_element_type=F32
            )
            for s in range(2):
                into[2 * i + s] = result[:, s * cols : (s + 1) * cols].astype(into.dtype)
            return carry

        lax.fori_loop(0, chips // 2, step, 0)

    products(1 - place.core, away)
    near = send(away, near_in, send_near, recv_near, place.partner)
    products(place.core, own)
    near.wait()
    far = []
    for d in range(1, chips):
        chip = place.chip_peer(d)
        pair[chip] = (own[chip] + near_in[chip].astype(F32)).astype(BF16)
        far.append(
            send(pair.at[chip], far_in.at[d], send_far.at[d], recv_far.at[d], place.tp_peer(d))
        )
    total = own[place.chip] + near_in[place.chip].astype(F32)
    for copy in far:
        copy.wait()
    for d in range(1, chips):
        total = total + far_in[d].astype(F32)
    return total


def project_scratch(place_shape, rows, steps):
    groups, width = place_shape
    exchange = pltpu.VMEM((groups, steps, rows // groups, 2 * LANES), BF16)
    sems = [pltpu.SemaphoreType.DMA((4, groups))] * 2
    return [exchange, exchange] + sems


def project(place, scaled, inverse_rms, weights, result_ref, scratch):
    out, into, send_sem, recv_sem = scratch
    groups, steps, part, wide = out.shape
    base, copies, where = 0, [], []
    for p, weight in enumerate(weights):
        count = weight.shape[1] // wide

        def products(j, carry, weight=weight, base=base):
            at = pl.ds(pl.multiple_of(j * wide, wide), wide)
            result = jnp.dot(scaled[...], weight[:, at], preferred_element_type=F32).astype(BF16)
            for k in range(groups):
                out[k, base + j] = result[k * part : (k + 1) * part]
            return carry

        lax.fori_loop(0, count, products, 0)
        span = pl.ds(base, count)
        copies.append(
            [
                send(
                    out.at[place.kv_index(d), span],
                    into.at[d, span],
                    send_sem.at[p, d],
                    recv_sem.at[p, d],
                    place.kv_peer(d),
                )
                for d in range(1, groups)
            ]
        )
        where.append((base, base + count))
        base += count
    factor = inverse_rms()
    for p, (low, high) in enumerate(where):
        for copy in copies[p]:
            copy.wait_recv()
        for j in range(low, high):
            total = out[place.kv, j].astype(F32)
            for d in range(1, groups):
                total = total + into[d, j].astype(F32)
            result_ref[:, j * wide : (j + 1) * wide] = total * factor
    for group in copies:
        for copy in group:
            copy.wait_send()


def take(refs, count):
    return [refs.pop(0) for _ in range(count)]


def load_all(sources, buffers, sem):
    copies = [
        pltpu.make_async_copy(source, buffer, sem.at[i])
        for i, (source, buffer) in enumerate(zip(sources, buffers))
    ]
    for copy in copies:
        copy.start()
    return copies


def first_kernel(shape, *refs):
    refs = list(refs)
    tokens, gain, mix_gain = take(refs, 3)
    sources = take(refs, 7)
    own_out, mix_out = take(refs, 2)
    buffers = take(refs, 7)
    (load_sem, own) = take(refs, 2)
    gather_a, gather_b = take(refs, 5), take(refs, 5)
    scale_a, scale_b = take(refs, 5), take(refs, 5)
    hidden_s, branch_s, project_s = take(refs, 7), take(refs, 9), take(refs, 4)
    place = Place(*shape)
    loads = load_all(sources, buffers, load_sem)
    w_gate, w_up, w_down = buffers[:3]
    place.barrier()
    blocks = gather_tp(place, tokens, gather_a)
    scaled, inverse_rms = scale(place, blocks, gain, scale_a)
    loads[0].wait()
    loads[1].wait()
    hidden = hidden_units(place, scaled, inverse_rms, w_gate, w_up, hidden_s)
    loads[2].wait()
    total = branch(place, hidden, w_down, 0.5, branch_s)
    own[...] = (tokens[...].astype(F32) + total).astype(BF16)
    own_out[...] = own[...]
    blocks = gather_tp(place, own, gather_b)
    scaled, inverse_rms = scale(place, blocks, mix_gain, scale_b)
    for load in loads[3:]:
        load.wait()
    project(place, scaled, inverse_rms, buffers[3:], mix_out, project_s)


def last_kernel(shape, *refs):
    refs = list(refs)
    heads, resid, gain = take(refs, 3)
    sources = take(refs, 4)
    (result,) = take(refs, 1)
    buffers = take(refs, 4)
    load_sem, own, joined, send_heads, recv_heads = take(refs, 5)
    gather_a, scale_a = take(refs, 5), take(refs, 5)
    hidden_s, branch_a, branch_b = take(refs, 7), take(refs, 9), take(refs, 9)
    place = Place(*shape)
    loads = load_all(sources, buffers, load_sem)
    w_out, w_gate, w_up, w_down = buffers
    place.barrier()
    part = heads.shape[0]
    rows = joined.at[pl.ds(pl.multiple_of(place.kv * part, part), part)]
    copies = [
        send(heads, rows, send_heads.at[d], recv_heads.at[d], place.kv_peer(d))
        for d in range(1, place.groups)
    ]
    rows[...] = heads[...]
    for copy in copies:
        copy.wait()
    loads[0].wait()
    total = branch(place, joined, w_out, 1.0, branch_a)
    own[...] = (resid[...].astype(F32) + total).astype(BF16)
    blocks = gather_tp(place, own, gather_a)
    scaled, inverse_rms = scale(place, blocks, gain, scale_a)
    loads[1].wait()
    loads[2].wait()
    hidden = hidden_units(place, scaled, inverse_rms, w_gate, w_up, hidden_s)
    loads[3].wait()
    total = branch(place, hidden, w_down, 0.5, branch_b)
    result[...] = (own[...].astype(F32) + total).astype(BF16)


def call(kernel, shape, small, large, outs, scratch, collective):
    vmem = pl.BlockSpec(memory_space=pltpu.VMEM)
    hbm = pl.BlockSpec(memory_space=pl.ANY)
    buffers = [pltpu.VMEM(w.shape, w.dtype) for w in large]
    return pl.pallas_call(
        lambda *refs: kernel(shape, *refs),
        name=kernel.__name__,
        out_shape=outs,
        in_specs=[vmem] * len(small) + [hbm] * len(large),
        out_specs=jax.tree.map(lambda _: vmem, outs),
        scratch_shapes=buffers + [pltpu.SemaphoreType.DMA((len(large),))] + scratch,
        compiler_params=pltpu.CompilerParams(
            collective_id=collective, has_side_effects=True, vmem_limit_bytes=VMEM_BYTES
        ),
    )(*small, *large)


def retain(mix, past_state, head_gain, key_cols, value_cols):
    row_count, local_heads = past_state.shape[:2]
    queries = mix[:, :key_cols]
    keys_now = mix[:, key_cols : 2 * key_cols]
    values_now = mix[:, 2 * key_cols : 2 * key_cols + value_cols]
    gate_now = mix[:, 2 * key_cols + value_cols :]
    queries = rotate(queries.reshape(row_count, local_heads, HEAD_K)) * HEAD_K ** (-0.5)
    keys_now = rotate(keys_now.reshape(row_count, local_heads, HEAD_K))
    values_now = values_now.reshape(row_count, local_heads, HEAD_V)
    head_level = (lax.axis_index("tp") * local_heads + jnp.arange(local_heads)).astype(F32)
    retained = 1.0 - jnp.exp2(-5.0 - 16.0 * head_level / (HEADS - 1))
    new_state = (
        retained[None, :, None, None] * past_state
        + keys_now[:, :, :, None] * values_now[:, :, None, :]
    )
    retrieved = jnp.einsum("bhk,bhkv->bhv", queries, new_state, precision=lax.Precision.HIGHEST)
    head_mean = jnp.mean(retrieved, axis=-1, keepdims=True)
    variance = jnp.mean(jnp.square(retrieved - head_mean), axis=-1, keepdims=True)
    normed = ((retrieved - head_mean) * lax.rsqrt(variance + EPS_GROUP)).reshape(
        row_count, local_heads * HEAD_V
    )
    return (jax.nn.silu(gate_now) * (normed * head_gain)).astype(BF16), new_state


def fused_shards(
    tokens,
    past_state,
    first_gain,
    first_gate,
    first_up,
    first_down,
    mix_gain,
    query_weight,
    key_weight,
    value_weight,
    output_gate_weight,
    head_gain,
    out_weight,
    second_gain,
    second_gate,
    second_up,
    second_down,
):
    shape = (lax.axis_size("kv"), lax.axis_size("tp"))
    rows, cols = tokens.shape
    part, units = rows // shape[0], first_gate.shape[1]
    mix_weights = (query_weight, key_weight, value_weight, output_gate_weight)
    mix_cols = sum(w.shape[1] for w in mix_weights)
    gather, scaling = gather_scratch(shape, rows, cols), scale_scratch(shape, rows, cols)
    hidden, branches = hidden_scratch(shape, rows, units), branch_scratch(shape, rows, cols)
    own = [pltpu.VMEM((rows, cols), BF16)]
    first, mix = call(
        first_kernel,
        shape,
        (tokens, first_gain[None], mix_gain[None]),
        (first_gate, first_up, first_down) + mix_weights,
        (
            jax.ShapeDtypeStruct((rows, cols), BF16),
            jax.ShapeDtypeStruct((part, mix_cols), F32),
        ),
        own
        + gather * 2
        + scaling * 2
        + hidden
        + branches
        + project_scratch(shape, rows, mix_cols // (2 * LANES)),
        0,
    )
    heads, new_state = retain(
        mix, past_state, head_gain, query_weight.shape[1], value_weight.shape[1]
    )
    mixed = call(
        last_kernel,
        shape,
        (heads, first, second_gain[None]),
        (out_weight, second_gate, second_up, second_down),
        jax.ShapeDtypeStruct((rows, cols), BF16),
        own
        + [pltpu.VMEM((rows, heads.shape[1]), BF16)]
        + [pltpu.SemaphoreType.DMA((shape[0],))] * 2
        + gather
        + scaling
        + hidden
        + branches * 2,
        1,
    )
    return mixed, new_state


def layer(*arrays):
    groups, width = lax.axis_size("kv"), lax.axis_size("tp")
    tokens, first_gate, mix_weights = arrays[0], arrays[3], arrays[7:11]
    rows, cols = tokens.shape
    whole_tiles = (
        groups > 1
        and width % 4 == 0
        and cols % LANES == 0
        and rows % (16 * groups) == 0
        and first_gate.shape[1] % LANES == 0
        and all(weight.shape[1] % (2 * LANES) == 0 for weight in mix_weights)
    )
    return fused_shards(*arrays) if whole_tiles else shards(*arrays)


def solution(mesh):
    in_specs = (
        P(None, ("kv", "tp")),
        P("kv", "tp", None, None),
        P("kv"),
        P("kv", "tp"),
        P("kv", "tp"),
        P("tp", "kv"),
        P("kv"),
        P("kv", "tp"),
        P("kv", "tp"),
        P("kv", "tp"),
        P("kv", "tp"),
        P("tp"),
        P("tp", "kv"),
        P("kv"),
        P("kv", "tp"),
        P("kv", "tp"),
        P("tp", "kv"),
    )
    out_specs = (P(None, ("kv", "tp")), P("kv", "tp", None, None))
    return jax.shard_map(layer, mesh=mesh, in_specs=in_specs, out_specs=out_specs, check_vma=False)
```

```python
import jax
import jax.numpy as jnp
from jax import lax
from jax.experimental import pallas as pl
from jax.experimental.pallas import tpu as pltpu
from jax.sharding import PartitionSpec as P

D = 4096
HEADS = 32
HEAD_K = 64
HEAD_V = 128
POS = 16384


EPS_RMS = 1e-06
EPS_GROUP = 1e-05
ROPE_BASE = 10000.0


def rotate(vectors):
    half_width = vectors.shape[-1] // 2
    frequency = ROPE_BASE ** (-jnp.arange(half_width, dtype=jnp.float32) / half_width)
    angles = POS * frequency
    cosine = jnp.cos(angles)
    sine_part = jnp.sin(angles)
    lower = vectors[..., :half_width]
    upper = vectors[..., half_width:]
    return jnp.concatenate(
        [lower * cosine - upper * sine_part, lower * sine_part + upper * cosine], axis=-1
    )


def activate(gate_sum, up_sum, summed):
    inverse_rms = lax.rsqrt(summed / D + EPS_RMS)[:, None]
    return (jax.nn.silu(gate_sum * inverse_rms) * (up_sum * inverse_rms)).astype(jnp.bfloat16)


def channel_mix(widened, gain, w_gate, w_up, w_down):
    widened_f = widened.astype(jnp.float32)
    scaled = (widened_f * gain).astype(jnp.bfloat16)
    squares = jnp.sum(widened_f * widened_f, axis=1)
    gate_part = jnp.dot(scaled, w_gate, preferred_element_type=jnp.float32)
    up_part = jnp.dot(scaled, w_up, preferred_element_type=jnp.float32)
    gate_sum, up_sum, summed = (
        lax.psum(gate_part.astype(jnp.bfloat16), "kv").astype(jnp.float32),
        lax.psum(up_part.astype(jnp.bfloat16), "kv").astype(jnp.float32),
        lax.psum(squares.astype(jnp.bfloat16), "kv").astype(jnp.float32),
    )
    return 0.5 * jnp.dot(
        activate(gate_sum, up_sum, summed), w_down, preferred_element_type=jnp.float32
    )


def token_mix(
    widened,
    past_state,
    gain,
    query_weight,
    key_weight,
    value_weight,
    output_gate_weight,
    head_gain,
    out_weight,
):
    widened_f = widened.astype(jnp.float32)
    scaled = (widened_f * gain).astype(jnp.bfloat16)
    squares = jnp.sum(widened_f * widened_f, axis=1)
    query_part = jnp.dot(scaled, query_weight, preferred_element_type=jnp.float32)
    key_part = jnp.dot(scaled, key_weight, preferred_element_type=jnp.float32)
    value_part = jnp.dot(scaled, value_weight, preferred_element_type=jnp.float32)
    gate_part = jnp.dot(scaled, output_gate_weight, preferred_element_type=jnp.float32)
    queries, keys_now, values_now, gate_now, summed = (
        lax.psum_scatter(
            query_part.astype(jnp.bfloat16), "kv", scatter_dimension=0, tiled=True
        ).astype(jnp.float32),
        lax.psum_scatter(
            key_part.astype(jnp.bfloat16), "kv", scatter_dimension=0, tiled=True
        ).astype(jnp.float32),
        lax.psum_scatter(
            value_part.astype(jnp.bfloat16), "kv", scatter_dimension=0, tiled=True
        ).astype(jnp.float32),
        lax.psum_scatter(
            gate_part.astype(jnp.bfloat16), "kv", scatter_dimension=0, tiled=True
        ).astype(jnp.float32),
        lax.psum_scatter(
            squares.astype(jnp.bfloat16), "kv", scatter_dimension=0, tiled=True
        ).astype(jnp.float32),
    )
    inverse_rms = lax.rsqrt(summed / D + EPS_RMS)[:, None]
    row_count = past_state.shape[0]
    local_heads = past_state.shape[1]
    queries = rotate((queries * inverse_rms).reshape(row_count, local_heads, HEAD_K)) * HEAD_K ** (
        -0.5
    )
    keys_now = rotate((keys_now * inverse_rms).reshape(row_count, local_heads, HEAD_K))
    values_now = (values_now * inverse_rms).reshape(row_count, local_heads, HEAD_V)
    gate_now = gate_now * inverse_rms
    head_level = (lax.axis_index("tp") * local_heads + jnp.arange(local_heads)).astype(jnp.float32)
    retained = 1.0 - jnp.exp2(-5.0 - 16.0 * head_level / (HEADS - 1))
    new_state = (
        retained[None, :, None, None] * past_state
        + keys_now[:, :, :, None] * values_now[:, :, None, :]
    )
    retrieved = jnp.einsum("bhk,bhkv->bhv", queries, new_state, precision=lax.Precision.HIGHEST)
    head_mean = jnp.mean(retrieved, axis=-1, keepdims=True)
    variance = jnp.mean(jnp.square(retrieved - head_mean), axis=-1, keepdims=True)
    normed = ((retrieved - head_mean) * lax.rsqrt(variance + EPS_GROUP)).reshape(
        row_count, local_heads * HEAD_V
    )
    mixed_heads = (jax.nn.silu(gate_now) * (normed * head_gain)).astype(jnp.bfloat16)
    projected = jnp.dot(
        lax.all_gather(mixed_heads, "kv", axis=0, tiled=True),
        out_weight,
        preferred_element_type=jnp.float32,
    )
    return (projected, new_state)


def shards(
    tokens,
    past_state,
    first_gain,
    first_gate,
    first_up,
    first_down,
    mix_gain,
    query_weight,
    key_weight,
    value_weight,
    output_gate_weight,
    head_gain,
    out_weight,
    second_gain,
    second_gate,
    second_up,
    second_down,
):

    def first_section(widened):
        return (channel_mix(widened, first_gain, first_gate, first_up, first_down), None)

    def middle_section(widened):
        return token_mix(
            widened,
            past_state,
            mix_gain,
            query_weight,
            key_weight,
            value_weight,
            output_gate_weight,
            head_gain,
            out_weight,
        )

    def last_section(widened):
        return (channel_mix(widened, second_gain, second_gate, second_up, second_down), None)

    sections = [first_section, middle_section, last_section]
    own_columns = tokens
    widened = lax.all_gather(tokens, "tp", axis=1, tiled=True)
    state_out = past_state
    for section_index in range(3):
        branch_out, produced = sections[section_index](widened)
        if produced is not None:
            state_out = produced
        own_piece = lax.psum_scatter(
            branch_out.astype(jnp.bfloat16), "tp", scatter_dimension=1, tiled=True
        ).astype(jnp.float32)
        own_columns = (own_columns.astype(jnp.float32) + own_piece).astype(jnp.bfloat16)
        if section_index < 2:
            widened = lax.all_gather(own_columns, "tp", axis=1, tiled=True)
    return (own_columns, state_out)


MESH = pl.DeviceIdType.MESH
LANES = 128
F32 = jnp.float32
BF16 = jnp.bfloat16
MIB = 1024 * 1024
FIRST_MIB, STATE_MIB, LAST_MIB = 54, 16, 54


def send(src, dst, send_sem, recv_sem, target):
    copy = pltpu.make_async_remote_copy(
        src_ref=src,
        dst_ref=dst,
        send_sem=send_sem,
        recv_sem=recv_sem,
        device_id=target,
        device_id_type=MESH,
    )
    copy.start()
    return copy


class Place:
    def __init__(self, groups, width):
        self.groups, self.width, self.chips = groups, width, width // 2
        self.kv = lax.axis_index("kv")
        self.tp = lax.axis_index("tp")
        self.chip = self.tp // 2
        self.core = lax.rem(self.tp, 2)
        self.partner = {"tp": 2 * self.chip + 1 - self.core}

    def chip_peer(self, d):
        return lax.rem(self.chip + d, self.chips)

    def tp_peer(self, d):
        return {"tp": 2 * self.chip_peer(d) + self.core}

    def tp_origin(self, d):
        return 2 * lax.rem(self.chip + self.chips - d, self.chips) + self.core

    def kv_index(self, d):
        return lax.rem(self.kv + d, self.groups)

    def kv_peer(self, d):
        return {"kv": self.kv_index(d)}

    def barrier(self):
        barrier = pltpu.get_barrier_semaphore()
        targets = [self.partner]
        targets += [self.tp_peer(d) for d in range(1, self.chips)]
        targets += [self.kv_peer(d) for d in range(1, self.groups)]
        for target in targets:
            pl.semaphore_signal(barrier, inc=1, device_id=target, device_id_type=MESH)
        pl.semaphore_wait(barrier, len(targets))


def gather_scratch(place_shape, rows, cols):
    groups, width = place_shape
    chips = width // 2
    sems = [pltpu.SemaphoreType.DMA((chips,))] * 4
    return [pltpu.VMEM((width, rows, cols), BF16)] + sems


def gather_tp(place, own, scratch):
    blocks, send_far, recv_far, send_near, recv_near = scratch
    me = place.tp
    far = [
        send(own, blocks.at[me], send_far.at[d], recv_far.at[d], place.tp_peer(d))
        for d in range(1, place.chips)
    ]
    near = [send(own, blocks.at[me], send_near.at[0], recv_near.at[0], place.partner)]
    blocks[me] = own[...]
    for d in range(1, place.chips):
        far[d - 1].wait_recv()
        block = blocks.at[place.tp_origin(d)]
        near.append(send(block, block, send_near.at[d], recv_near.at[d], place.partner))
    for copy in near:
        copy.wait_recv()
    for copy in far + near:
        copy.wait_send()
    return blocks


def scale_scratch(place_shape, rows, cols):
    groups, width = place_shape
    sems = [pltpu.SemaphoreType.DMA((groups,))] * 2
    return [
        pltpu.VMEM((rows, width * cols), BF16),
        pltpu.VMEM((groups, rows // groups, LANES), BF16),
        pltpu.VMEM((groups, rows // groups, LANES), BF16),
    ] + sems


def scale(place, blocks, gain, scratch):
    scaled, sq_out, sq_in, send_sem, recv_sem = scratch
    width, rows, cols = blocks.shape
    part = rows // place.groups
    total = jnp.zeros((rows, 1), F32)
    for t in range(width):
        block = blocks[t].astype(F32)
        at = slice(t * cols, (t + 1) * cols)
        scaled[:, at] = (block * gain[:, at]).astype(BF16)
        total = total + jnp.sum(block * block, axis=1, keepdims=True)
    high = total.astype(BF16).astype(F32)
    low = total - high
    lane = lax.broadcasted_iota(jnp.int32, (rows, LANES), 1)
    both = jnp.where(lane < LANES // 2, high, low).astype(BF16)
    for k in range(place.groups):
        sq_out[k] = both[k * part : (k + 1) * part]
    copies = [
        send(
            sq_out.at[place.kv_index(d)],
            sq_in.at[d],
            send_sem.at[d],
            recv_sem.at[d],
            place.kv_peer(d),
        )
        for d in range(1, place.groups)
    ]

    def inverse_rms():
        for copy in copies:
            copy.wait()
        both = sq_out[place.kv].astype(F32)
        for d in range(1, place.groups):
            both = both + sq_in[d].astype(F32)
        summed = jnp.sum(both, axis=1, keepdims=True) / (LANES // 2)
        return lax.rsqrt(summed / D + EPS_RMS)

    return scaled, inverse_rms


def spans(count, pieces):
    cuts = [count * i // pieces for i in range(pieces + 1)]
    return [(a, b) for a, b in zip(cuts, cuts[1:]) if b > a]


FF_PIECES = 3


def hidden_scratch(place_shape, rows, units):
    groups, width = place_shape
    part, tiles = rows // groups, units // LANES
    pair = pltpu.VMEM((2, 2, tiles, part, LANES), BF16)
    single = pltpu.VMEM((2, tiles, part, LANES), BF16)
    sems = [pltpu.SemaphoreType.DMA((FF_PIECES, 2, 3))] * 2
    sems += [pltpu.SemaphoreType.DMA((FF_PIECES, 4))] * 2
    everything = pltpu.VMEM((2, groups, tiles, part, LANES), BF16)
    return [everything, pair, single, single, pltpu.VMEM((rows, units), BF16)] + sems


def hidden_units(place, scaled, inverse_rms, w_gate, w_up, scratch):
    out, into, sums, last, hidden, send_part, recv_part, send_hid, recv_hid = scratch
    rows, units = hidden.shape
    groups = place.groups
    part, tiles = rows // groups, units // LANES
    pieces = spans(tiles, FF_PIECES)
    far_y, far_x = place.kv // 2, lax.rem(place.kv, 2)
    along_x = 2 * far_y + 1 - far_x
    along_y = 2 * (1 - far_y) + far_x
    diagonal = 3 - place.kv
    turns = ((along_x, along_y), (along_y, along_x))

    def lanes(j):
        return pl.ds(pl.multiple_of(j * LANES, LANES), LANES)

    def rows_of(k):
        return pl.ds(pl.multiple_of(k * part, part), part)

    def products(j, carry):
        weights = jnp.concatenate([w_gate[:, lanes(j)], w_up[:, lanes(j)]], axis=1)
        result = jnp.dot(scaled[...], weights, preferred_element_type=F32).astype(BF16)
        for k in range(groups):
            for side in range(2):
                out[side, k, j] = result[
                    k * part : (k + 1) * part, side * LANES : (side + 1) * LANES
                ]
        return carry

    passing, direct, summed, shared, passed = {}, {}, {}, {}, {}
    for p, (low, high) in enumerate(pieces):
        lax.fori_loop(low, high, products, 0)
        span = pl.ds(low, high - low)
        for side in range(2):
            near = turns[side][0]
            for which, block, store in ((1, diagonal, passing), (0, near, direct)):
                store[p, side] = send(
                    out.at[side, block, span],
                    into.at[side, which, span],
                    send_part.at[p, side, which],
                    recv_part.at[p, side, which],
                    {"kv": near},
                )

    def pass_on(p):
        low, high = pieces[p]
        span = pl.ds(low, high - low)
        for side in range(2):
            next_one = turns[side][1]
            passing[p, side].wait_recv()

            def add(j, carry, side=side, next_one=next_one):
                total = out[side, next_one, j].astype(F32) + into[side, 1, j].astype(F32)
                sums[side, j] = total.astype(BF16)
                return carry

            lax.fori_loop(low, high, add, 0)
            summed[p, side] = send(
                sums.at[side, span],
                last.at[side, span],
                send_part.at[p, side, 2],
                recv_part.at[p, side, 2],
                {"kv": next_one},
            )

    def activate_piece(p, factor):
        low, high = pieces[p]
        for side in range(2):
            direct[p, side].wait_recv()
            summed[p, side].wait_recv()

        def activation(j, carry):
            both = [
                factor
                * (
                    out[side, place.kv, j].astype(F32)
                    + into[side, 0, j].astype(F32)
                    + last[side, j].astype(F32)
                )
                for side in range(2)
            ]
            value = both[0] / (1.0 + jnp.exp(-both[0])) * both[1]
            hidden[rows_of(place.kv), lanes(j)] = value.astype(BF16)
            return carry

        lax.fori_loop(low, high, activation, 0)
        block = hidden.at[rows_of(place.kv), low * LANES : high * LANES]
        for i, target in enumerate((along_x, along_y)):
            shared[p, i] = send(
                block, block, send_hid.at[p, i], recv_hid.at[p, i], {"kv": target}
            )

    def relay(p):
        low, high = pieces[p]
        middle = (low + high) // 2
        halves = ((low, middle), (middle, high))
        for i, (origin, target) in enumerate(turns):
            shared[p, i].wait_recv()
            start, end = halves[i]
            block = hidden.at[rows_of(origin), start * LANES : end * LANES]
            passed[p, i] = send(
                block, block, send_hid.at[p, 2 + i], recv_hid.at[p, 2 + i], {"kv": target}
            )

    factor = inverse_rms()
    count = len(pieces)
    for stage in range(count + 2):
        if stage < count:
            pass_on(stage)
        if 0 <= stage - 1 < count:
            activate_piece(stage - 1, factor)
        if 0 <= stage - 2:
            relay(stage - 2)
    for copy in passed.values():
        copy.wait()
    for group in (passing, direct, summed, shared):
        for copy in group.values():
            copy.wait_send()
    return hidden


def branch_scratch(place_shape, rows, cols):
    groups, width = place_shape
    chips = width // 2
    half = (chips, rows, cols)
    sems = [pltpu.SemaphoreType.DMA((chips,))] * 2
    near = [pltpu.SemaphoreType.DMA] * 2
    return [
        pltpu.VMEM(half, BF16),
        pltpu.VMEM(half, BF16),
        pltpu.VMEM(half, F32),
        pltpu.VMEM(half, BF16),
        pltpu.VMEM(half, BF16),
    ] + near + sems


def branch(place, left, weight, factor, scratch):
    away, near_in, own, pair, far_in, send_near, recv_near, send_far, recv_far = scratch
    chips, rows, cols = away.shape

    def products(core, into):
        def step(i, carry):
            columns = [
                weight[:, pl.ds(pl.multiple_of((2 * (2 * i + s) + core) * cols, cols), cols)]
                for s in range(2)
            ]
            result = factor * jnp.dot(
                left[...], jnp.concatenate(columns, axis=1), preferred_element_type=F32
            )
            for s in range(2):
                into[2 * i + s] = result[:, s * cols : (s + 1) * cols].astype(into.dtype)
            return carry

        lax.fori_loop(0, chips // 2, step, 0)

    products(1 - place.core, away)
    near = send(away, near_in, send_near, recv_near, place.partner)
    products(place.core, own)
    near.wait()
    far = []
    for d in range(1, chips):
        chip = place.chip_peer(d)
        pair[chip] = (own[chip] + near_in[chip].astype(F32)).astype(BF16)
        far.append(
            send(pair.at[chip], far_in.at[d], send_far.at[d], recv_far.at[d], place.tp_peer(d))
        )
    total = own[place.chip] + near_in[place.chip].astype(F32)
    for copy in far:
        copy.wait()
    for d in range(1, chips):
        total = total + far_in[d].astype(F32)
    return total


def project_scratch(place_shape, rows, steps):
    groups, width = place_shape
    exchange = pltpu.VMEM((groups, steps, rows // groups, 2 * LANES), BF16)
    sems = [pltpu.SemaphoreType.DMA((4, groups))] * 2
    return [exchange, exchange] + sems


def project(place, scaled, inverse_rms, weights, result_ref, scratch):
    out, into, send_sem, recv_sem = scratch
    groups, steps, part, wide = out.shape
    base, copies, where = 0, [], []
    for p, weight in enumerate(weights):
        count = weight.shape[1] // wide

        def products(j, carry, weight=weight, base=base):
            at = pl.ds(pl.multiple_of(j * wide, wide), wide)
            result = jnp.dot(scaled[...], weight[:, at], preferred_element_type=F32).astype(BF16)
            for k in range(groups):
                out[k, base + j] = result[k * part : (k + 1) * part]
            return carry

        lax.fori_loop(0, count, products, 0)
        span = pl.ds(base, count)
        copies.append(
            [
                send(
                    out.at[place.kv_index(d), span],
                    into.at[d, span],
                    send_sem.at[p, d],
                    recv_sem.at[p, d],
                    place.kv_peer(d),
                )
                for d in range(1, groups)
            ]
        )
        where.append((base, base + count))
        base += count
    factor = inverse_rms()
    for p, (low, high) in enumerate(where):
        for copy in copies[p]:
            copy.wait_recv()
        for j in range(low, high):
            total = out[place.kv, j].astype(F32)
            for d in range(1, groups):
                total = total + into[d, j].astype(F32)
            result_ref[:, j * wide : (j + 1) * wide] = total * factor
    for group in copies:
        for copy in group:
            copy.wait_send()


def take(refs, count):
    return [refs.pop(0) for _ in range(count)]


def load_all(sources, buffers, sem):
    copies = [
        pltpu.make_async_copy(source, buffer, sem.at[i])
        for i, (source, buffer) in enumerate(zip(sources, buffers))
    ]
    for copy in copies:
        copy.start()
    return copies


def first_kernel(shape, *refs):
    refs = list(refs)
    tokens, gain, mix_gain = take(refs, 3)
    sources = take(refs, 7)
    own_out, mix_out = take(refs, 2)
    buffers = take(refs, 7)
    (load_sem, own) = take(refs, 2)
    gather_a, gather_b = take(refs, 5), take(refs, 5)
    scale_a, scale_b = take(refs, 5), take(refs, 5)
    hidden_s, branch_s, project_s = take(refs, 9), take(refs, 9), take(refs, 4)
    place = Place(*shape)
    loads = load_all(sources, buffers, load_sem)
    w_gate, w_up, w_down = buffers[:3]
    place.barrier()
    blocks = gather_tp(place, tokens, gather_a)
    scaled, inverse_rms = scale(place, blocks, gain, scale_a)
    loads[0].wait()
    loads[1].wait()
    hidden = hidden_units(place, scaled, inverse_rms, w_gate, w_up, hidden_s)
    loads[2].wait()
    total = branch(place, hidden, w_down, 0.5, branch_s)
    own[...] = (tokens[...].astype(F32) + total).astype(BF16)
    own_out[...] = own[...]
    blocks = gather_tp(place, own, gather_b)
    scaled, inverse_rms = scale(place, blocks, mix_gain, scale_b)
    for load in loads[3:]:
        load.wait()
    project(place, scaled, inverse_rms, buffers[3:], mix_out, project_s)


def last_kernel(shape, *refs):
    refs = list(refs)
    heads, resid, gain = take(refs, 3)
    sources = take(refs, 4)
    (result,) = take(refs, 1)
    buffers = take(refs, 4)
    load_sem, own, joined, send_heads, recv_heads = take(refs, 5)
    gather_a, scale_a = take(refs, 5), take(refs, 5)
    hidden_s, branch_a, branch_b = take(refs, 9), take(refs, 9), take(refs, 9)
    place = Place(*shape)
    loads = load_all(sources, buffers, load_sem)
    w_out, w_gate, w_up, w_down = buffers
    place.barrier()
    part = heads.shape[0]
    rows = joined.at[pl.ds(pl.multiple_of(place.kv * part, part), part)]
    copies = [
        send(heads, rows, send_heads.at[d], recv_heads.at[d], place.kv_peer(d))
        for d in range(1, place.groups)
    ]
    rows[...] = heads[...]
    for copy in copies:
        copy.wait()
    loads[0].wait()
    total = branch(place, joined, w_out, 1.0, branch_a)
    own[...] = (resid[...].astype(F32) + total).astype(BF16)
    blocks = gather_tp(place, own, gather_a)
    scaled, inverse_rms = scale(place, blocks, gain, scale_a)
    loads[1].wait()
    loads[2].wait()
    hidden = hidden_units(place, scaled, inverse_rms, w_gate, w_up, hidden_s)
    loads[3].wait()
    total = branch(place, hidden, w_down, 0.5, branch_b)
    result[...] = (own[...].astype(F32) + total).astype(BF16)


def call(kernel, shape, small, large, outs, scratch, collective, limit):
    vmem = pl.BlockSpec(memory_space=pltpu.VMEM)
    hbm = pl.BlockSpec(memory_space=pltpu.HBM)
    buffers = [pltpu.VMEM(w.shape, w.dtype) for w in large]
    return pl.pallas_call(
        lambda *refs: kernel(shape, *refs),
        name=kernel.__name__,
        out_shape=outs,
        in_specs=[vmem] * len(small) + [hbm] * len(large),
        out_specs=jax.tree.map(lambda _: vmem, outs),
        scratch_shapes=buffers + [pltpu.SemaphoreType.DMA((len(large),))] + scratch,
        cost_estimate=pl.CostEstimate(
            flops=60_000_000_000, bytes_accessed=100_000_000, transcendentals=0
        ),
        compiler_params=pltpu.CompilerParams(
            collective_id=collective, has_side_effects=True, vmem_limit_bytes=limit * MIB
        ),
    )(*small, *large)


def turned(vectors, cosine, sine):
    width = vectors.shape[1]
    half = HEAD_K // 2
    lane = lax.broadcasted_iota(jnp.int32, vectors.shape, 1)
    lower = lax.rem(lane, HEAD_K) < half
    other = jnp.where(
        lower, pltpu.roll(vectors, width - half, 1), pltpu.roll(vectors, half, 1)
    )
    return vectors * cosine + other * sine


def retain_kernel(mix, past, cosine, sine, retained, head_gain, heads, new_state, retrieved):
    count, local_heads = past.shape[:2]
    key_cols, value_cols = local_heads * HEAD_K, local_heads * HEAD_V
    queries = turned(mix[:, :key_cols], cosine[...], sine[...]) * HEAD_K ** (-0.5)
    keys_now = turned(mix[:, key_cols : 2 * key_cols], cosine[...], sine[...])
    queries, keys_now = queries.T, keys_now.T
    for b in range(count):
        for h in range(local_heads):
            entries = slice(h * HEAD_K, (h + 1) * HEAD_K)
            lanes = slice(h * HEAD_V, (h + 1) * HEAD_V)
            at = 2 * key_cols + h * HEAD_V
            values_now = mix[b : b + 1, at : at + HEAD_V]
            new = retained[:, lanes] * past[b, h] + keys_now[entries, b : b + 1] * values_now
            new_state[b, h] = new
            retrieved[b : b + 1, lanes] = jnp.sum(
                queries[entries, b : b + 1] * new, axis=0, keepdims=True
            )
    for h in range(local_heads):
        lanes = slice(h * HEAD_V, (h + 1) * HEAD_V)
        at = 2 * key_cols + value_cols + h * HEAD_V
        gate = mix[:, at : at + HEAD_V]
        found = retrieved[:, lanes]
        off = found - jnp.mean(found, axis=1, keepdims=True)
        variance = jnp.mean(off * off, axis=1, keepdims=True)
        normed = off * lax.rsqrt(variance + EPS_GROUP) * head_gain[:, lanes]
        heads[:, lanes] = (gate / (1.0 + jnp.exp(-gate)) * normed).astype(BF16)


def retain(mix, past_state, head_gain):
    row_count, local_heads = past_state.shape[:2]
    half = HEAD_K // 2
    frequency = ROPE_BASE ** (-jnp.arange(half, dtype=F32) / half)
    angles = POS * frequency
    sine_part = jnp.sin(angles)
    cosine = jnp.tile(jnp.cos(angles), 2 * local_heads)[None]
    sine = jnp.tile(jnp.concatenate([-sine_part, sine_part]), local_heads)[None]
    head_level = (lax.axis_index("tp") * local_heads + jnp.arange(local_heads)).astype(F32)
    retained = jnp.repeat(1.0 - jnp.exp2(-5.0 - 16.0 * head_level / (HEADS - 1)), HEAD_V)[None]
    block = 8
    state = pl.BlockSpec((block,) + past_state.shape[1:], lambda i: (i, 0, 0, 0))

    def rows(width):
        return pl.BlockSpec((block, width), lambda i: (i, 0))

    def whole(array):
        return pl.BlockSpec(array.shape, lambda i: (0, 0))

    value_cols = local_heads * HEAD_V
    gain = head_gain[None]
    return pl.pallas_call(
        retain_kernel,
        grid=(row_count // block,),
        out_shape=(
            jax.ShapeDtypeStruct((row_count, value_cols), BF16),
            jax.ShapeDtypeStruct(past_state.shape, F32),
        ),
        in_specs=[rows(mix.shape[1]), state]
        + [whole(array) for array in (cosine, sine, retained, gain)],
        out_specs=(rows(value_cols), state),
        scratch_shapes=[pltpu.VMEM((block, value_cols), F32)],
        compiler_params=pltpu.CompilerParams(vmem_limit_bytes=STATE_MIB * MIB),
        cost_estimate=pl.CostEstimate(
            flops=5 * past_state.size, bytes_accessed=8 * past_state.size, transcendentals=0
        ),
    )(mix, past_state, cosine, sine, retained, gain)


def fused_shards(
    tokens,
    past_state,
    first_gain,
    first_gate,
    first_up,
    first_down,
    mix_gain,
    query_weight,
    key_weight,
    value_weight,
    output_gate_weight,
    head_gain,
    out_weight,
    second_gain,
    second_gate,
    second_up,
    second_down,
):
    shape = (lax.axis_size("kv"), lax.axis_size("tp"))
    rows, cols = tokens.shape
    part, units = rows // shape[0], first_gate.shape[1]
    mix_weights = (query_weight, key_weight, value_weight, output_gate_weight)
    mix_cols = sum(w.shape[1] for w in mix_weights)
    gather, scaling = gather_scratch(shape, rows, cols), scale_scratch(shape, rows, cols)
    hidden, branches = hidden_scratch(shape, rows, units), branch_scratch(shape, rows, cols)
    own = [pltpu.VMEM((rows, cols), BF16)]
    first, mix = call(
        first_kernel,
        shape,
        (tokens, first_gain[None], mix_gain[None]),
        (first_gate, first_up, first_down) + mix_weights,
        (
            jax.ShapeDtypeStruct((rows, cols), BF16),
            jax.ShapeDtypeStruct((part, mix_cols), F32),
        ),
        own
        + gather * 2
        + scaling * 2
        + hidden
        + branches
        + project_scratch(shape, rows, mix_cols // (2 * LANES)),
        0,
        FIRST_MIB,
    )
    heads, new_state = retain(mix, past_state, head_gain)
    mixed = call(
        last_kernel,
        shape,
        (heads, first, second_gain[None]),
        (out_weight, second_gate, second_up, second_down),
        jax.ShapeDtypeStruct((rows, cols), BF16),
        own
        + [pltpu.VMEM((rows, heads.shape[1]), BF16)]
        + [pltpu.SemaphoreType.DMA((shape[0],))] * 2
        + gather
        + scaling
        + hidden
        + branches * 2,
        1,
        LAST_MIB,
    )
    return mixed, new_state


def layer(*arrays):
    groups, width = lax.axis_size("kv"), lax.axis_size("tp")
    tokens, first_gate, mix_weights = arrays[0], arrays[3], arrays[7:11]
    rows, cols = tokens.shape
    whole_tiles = (
        groups == 4
        and width % 4 == 0
        and cols % LANES == 0
        and rows % (16 * groups) == 0
        and first_gate.shape[1] % LANES == 0
        and all(weight.shape[1] % (2 * LANES) == 0 for weight in mix_weights)
    )
    return fused_shards(*arrays) if whole_tiles else shards(*arrays)


def solution(mesh):
    in_specs = (
        P(None, ("kv", "tp")),
        P("kv", "tp", None, None),
        P("kv"),
        P("kv", "tp"),
        P("kv", "tp"),
        P("tp", "kv"),
        P("kv"),
        P("kv", "tp"),
        P("kv", "tp"),
        P("kv", "tp"),
        P("kv", "tp"),
        P("tp"),
        P("tp", "kv"),
        P("kv"),
        P("kv", "tp"),
        P("kv", "tp"),
        P("tp", "kv"),
    )
    out_specs = (P(None, ("kv", "tp")), P("kv", "tp", None, None))
    return jax.shard_map(layer, mesh=mesh, in_specs=in_specs, out_specs=out_specs, check_vma=False)
```
